32 devices in a mesh: gr: 2 (over y), fs: 4 (over z), tp: 4 (over x, core).
Axes of the slice: x: 2, y: 2, z: 4, core: 2. Of those that a mesh axis runs over, the one named last changes fastest.
Arguments:
- tokens: bfloat16 [4096, 2048], P(('gr', 'tp'), 'fs'), may hold values from -6 to 6
- routes: int32 [4096, 2], P(('gr', 'tp')), may hold values from 0 to 7, all different within a row; in each aligned block of 512 rows (0 to 511, 512 to 1023, ...) at most 192 rows name the same one
- route_weight: float32 [4096, 2], P(('gr', 'tp')), may hold values from 0.25 to 1
- norm_gain: float32 [2048], P(('gr', 'fs')), may hold values from 0.1 to 1.9
- gate_master: float32 [8, 2048, 2816], P(None, ('gr', 'fs'), 'tp'), may hold values from -0.125 to 0.125
- up_master: float32 [8, 2048, 2816], P(None, ('gr', 'fs'), 'tp'), may hold values from -0.125 to 0.125
- down_master: float32 [8, 2048, 2816], P(None, ('gr', 'fs'), 'tp'), may hold values from -0.109375 to 0.109375
Outputs:
- mixed_output: bfloat16 [4096, 2048], P(('gr', 'tp'), 'fs')
- gate_serving: bfloat16 [8, 2048, 2816], P('tp', None, 'fs')
- up_serving: bfloat16 [8, 2048, 2816], P('tp', None, 'fs')
- down_serving: bfloat16 [8, 2048, 2816], P('tp', None, 'fs')
The draws below stay inside these ranges and needn't reach their ends.
Inputs may be any that keep to these rules, and one draw needn't show every extreme that they name: `routes`: each row names two different experts. Within the rows of one block of 512 tokens (one index of gr+tp) no expert is named by more than 192 rows, and in some blocks one expert is named by exactly 192.
All inputs are finite; a program needn't handle non-finite values.
Results may differ from the reference program's by a relative error of at most 0.0082.
Values may be sent and summed in bfloat16 or wider, within the bound.
A program may use at most 128 MiB of HBM per device.

```python
import math
import jax
import jax.numpy as jnp
import numpy as np
from jax import lax

D = 2048
EFF = 2816
EXPERTS = 8
TOK_DEV = 512
CAP = 192
TOKENS = 4096


def shard_levels(stream_key, dims, cuts, low, largest):
    loudness, own = 1.0, jax.random.fold_in(stream_key, 6)
    for dim, blocks in cuts:
        steps = jnp.exp(jax.random.uniform(jax.random.fold_in(own, dim), (blocks,), jnp.float32, low / len(cuts), largest / len(cuts)))
        loudness = loudness * jnp.repeat(steps, dims[dim] // blocks).reshape([-1 if axis == dim else 1 for axis in range(len(dims))])
    return loudness


def deal_out(stream_key, own, number, rows, count, top, bound, skew):
    ranking = jax.random.permutation(stream_key, count)
    heavy_load, common = portions_of(count, rows * top, bound, skew, True), portions_of(count, rows * top, bound, skew, False)
    places = jnp.arange(count)

    def named(tallies, rotation):
        used = int((tallies > 0).sum())
        fixed = max(1, used // 4)
        passed = fixed + (places - fixed + rotation * (used - fixed)) % max(1, count - fixed)
        return jnp.zeros((count,), jnp.int32).at[ranking[jnp.where(places < fixed, places, passed)]].set(jnp.asarray(tallies, jnp.int32))

    tallies = jnp.where(number % 4 == 0, named(heavy_load, number // 4), named(common, number - number // 4 - 1))
    mixed = jax.random.permutation(jax.random.fold_in(own, 3), count)
    source_of, sink = mixed[0:count // 2 * 2:2], mixed[1:count // 2 * 2:2]
    slack = jnp.minimum(tallies[source_of] - 1, bound - tallies[sink]) // 2
    slack = jnp.where((source_of == ranking[0]) | (sink == ranking[0]) | (tallies[sink] == 0), 0, jnp.maximum(slack, 0))
    passed = jax.random.randint(jax.random.fold_in(own, 4), (count // 2,), 0, 1 << 20) % (slack + 1)
    tallies = tallies.at[source_of].add(-passed).at[sink].add(passed)
    members = jnp.searchsorted(jnp.cumsum(tallies), jnp.arange(rows * top), side="right").astype(jnp.int32)
    grid = members.reshape(top, rows).T
    grid = grid[jax.random.permutation(jax.random.fold_in(own, 1), rows)]
    rotation = jax.random.randint(jax.random.fold_in(own, 2), (rows, 1), 0, top)
    return jnp.take_along_axis(grid, (jnp.arange(top)[None, :] + rotation) % top, axis=1)


def portions_of(count, total, reach, slope, full):
    portions = [(1 << 20) // math.isqrt(standing ** slope) + 1 for standing in range(1, count + 1)]
    largest = reach if full else min(reach, max(-(-total // count), total * portions[0] // sum(portions)))
    least = 1 if total - largest >= count - 1 else 0
    holding, rest = [largest] + [least] * (count - 1), total - largest - least * (count - 1)
    while rest > 0:
        candidates = [i for i in range(1, count) if holding[i] < largest] or [i for i in range(1, count) if holding[i] < reach]
        whole, left = sum([portions[i] for i in candidates]), rest
        for i in candidates:
            addition = min(reach - holding[i], max(1, left * portions[i] // whole), rest)
            holding[i] = holding[i] + addition
            rest = rest - addition
    return np.array(holding)


def normal_values(key, shape, deviation, bound, cuts=(), held_as=jnp.bfloat16):
    values = deviation * jax.random.normal(key, shape, jnp.float32)
    if cuts:
        values = values * shard_levels(key, shape, cuts, -0.22, 0.18)
    return jnp.clip(values, -bound, bound).astype(held_as)


def setup_inputs(seed: int = 0) -> dict:
    arg_keys = jax.random.split(jax.random.key(seed), 8)
    tokens = normal_values(arg_keys[0], (TOKENS, D), 1.0, 6.0, ((0, 8), (1, 4)))
    routes_keys = jax.random.split(jax.random.fold_in(arg_keys[1], 1), TOKENS // TOK_DEV)
    routes_turns = jax.random.permutation(jax.random.fold_in(arg_keys[1], 3), TOKENS // TOK_DEV)
    routes = jax.vmap(lambda own, number: deal_out(jax.random.fold_in(arg_keys[1], 2), own, number, TOK_DEV, EXPERTS, 2, CAP, 1))(routes_keys, routes_turns).reshape((TOKENS, 2))
    route_weight = jnp.clip(jnp.exp(math.log(1.0) - 1.3862944 * jax.random.uniform(arg_keys[2], (TOKENS, 2), jnp.float32) ** shard_levels(arg_keys[2], (TOKENS, 2), ((0, 8),), -0.2, 0.2)), 0.25, 1.0)
    norm_gain = jnp.clip(1.0 + 0.18 * jax.random.normal(arg_keys[3], (D,), jnp.float32), 0.1, 1.9)
    gate_master = normal_values(arg_keys[4], (EXPERTS, D, EFF), D ** -0.5, 0.125, ((1, 8), (2, 4)), jnp.float32)
    up_master = normal_values(arg_keys[5], (EXPERTS, D, EFF), D ** -0.5, 0.125, ((1, 8), (2, 4)), jnp.float32)
    down_master = normal_values(arg_keys[6], (EXPERTS, D, EFF), EFF ** -0.5, 0.109375, ((1, 8), (2, 4)), jnp.float32)
    return {"tokens": tokens, "routes": routes, "route_weight": route_weight, "norm_gain": norm_gain, "gate_master": gate_master, "up_master": up_master, "down_master": down_master}


norm_eps = 1e-06

def slot_table(routes, experts, capacity):
    flat_routes = routes.reshape(-1)
    onehot = (flat_routes[:, None] == jnp.arange(experts, dtype=jnp.int32)[None, :]).astype(jnp.int32)
    running = jnp.cumsum(onehot, axis=0)
    slot_index = lax.optimization_barrier(jnp.sum(onehot * (running - 1), axis=1))
    return (flat_routes * capacity + slot_index).astype(jnp.int32)

def reference(tokens, routes, route_weight, norm_gain, gate_master, up_master, down_master):
    gate_serving = (gate_master * norm_gain[None, :, None]).astype(jnp.bfloat16)
    up_serving = (up_master * norm_gain[None, :, None]).astype(jnp.bfloat16)
    down_serving = down_master.astype(jnp.bfloat16)
    blocks = TOKENS // TOK_DEV
    as_float = tokens.astype(jnp.float32)
    normed = (as_float * lax.rsqrt(lax.optimization_barrier(jnp.mean(as_float * as_float, axis=1, keepdims=True)) + norm_eps)).astype(jnp.bfloat16)
    normed = normed.reshape(blocks, TOK_DEV, D)
    route_blocks = routes.reshape(blocks, TOK_DEV, 2)

    def find_slots(block_routes):
        return slot_table(block_routes, EXPERTS, CAP)
    placing = jax.vmap(find_slots)(route_blocks)
    slot_rows = jnp.arange(EXPERTS * CAP, dtype=jnp.int32)

    def pick(block_places):
        return (slot_rows[:, None] == block_places[None, :]).reshape(EXPERTS * CAP, TOK_DEV, 2)

    def dispatch(block_places, block_rows):
        route_table = lax.optimization_barrier(jnp.sum(pick(block_places).astype(jnp.float32), axis=2)).astype(jnp.bfloat16)
        return jnp.dot(route_table, block_rows, preferred_element_type=jnp.float32).astype(jnp.bfloat16)
    outgoing = jax.vmap(dispatch)(placing, normed)
    outgoing = outgoing.reshape(blocks, EXPERTS, CAP, D).transpose(1, 0, 2, 3).reshape(EXPERTS, blocks * CAP, D)

    def expert(inputs):
        slots, w_gate, w_up, w_down = inputs
        gate_acc = jnp.dot(slots, w_gate, preferred_element_type=jnp.float32)
        up_acc = jnp.dot(slots, w_up, preferred_element_type=jnp.float32)
        hidden = (jax.nn.silu(gate_acc) * up_acc).astype(jnp.bfloat16)
        return lax.dot_general(hidden, w_down, (((1,), (1,)), ((), ())), preferred_element_type=jnp.float32)
    outputs = lax.map(expert, (outgoing, gate_serving, up_serving, down_serving))
    outputs = outputs.reshape(EXPERTS, blocks, CAP, D).transpose(1, 0, 2, 3).reshape(blocks, EXPERTS * CAP, D)

    def combine(block_places, weight, produced):
        weights = lax.optimization_barrier(jnp.sum(jnp.where(pick(block_places), weight.reshape(1, TOK_DEV, 2), 0.0), axis=2))
        return lax.dot_general(weights, produced, (((0,), (0,)), ((), ())), precision=lax.Precision.HIGHEST, preferred_element_type=jnp.float32)
    mixed_output = jax.vmap(combine)(placing, route_weight.reshape(blocks, TOK_DEV, 2), outputs)
    return (mixed_output.reshape(TOKENS, D).astype(jnp.bfloat16), gate_serving, up_serving, down_serving)
```

```python
import functools

import jax
import jax.numpy as jnp
from jax import lax
from jax.experimental import pallas as pl
from jax.experimental.pallas import tpu as pltpu
from jax.sharding import PartitionSpec as P

norm_eps = 1e-06
MESH = pl.DeviceIdType.MESH


def slot_table(routes, experts, capacity):
    flat_routes = routes.reshape(-1)
    onehot = (flat_routes[:, None] == jnp.arange(experts, dtype=jnp.int32)[None, :]).astype(
        jnp.int32
    )
    running = jnp.cumsum(onehot, axis=0)
    slot_index = jnp.sum(onehot * (running - 1), axis=1)
    return flat_routes * capacity + slot_index


def spread_kernel(sizes, count, *refs):
    gr, fs, tp, sub, local_experts, rows = sizes
    ins, outs, relays = refs[:count], refs[count : 2 * count], refs[2 * count : 3 * count]
    bounce, tp_send, tp_recv, fs_send, fs_recv, gr_send, gr_recv, load_sem, store_sem = refs[
        3 * count :
    ]
    g, f, t = lax.axis_index("gr"), lax.axis_index("fs"), lax.axis_index("tp")
    blocks = [(w, j) for j in range(local_experts) for w in range(count)]

    barrier = pltpu.get_barrier_semaphore()
    for axis, me, size in (("gr", g, gr), ("fs", f, fs), ("tp", t, tp)):
        for d in range(1, size):
            pl.semaphore_signal(
                barrier, inc=1, device_id={axis: lax.rem(me + d, size)}, device_id_type=MESH
            )
    pl.semaphore_wait(barrier, gr + fs + tp - 3)

    def out_rows(c, group, source):
        w, j = blocks[c]
        start = pl.multiple_of((group * fs + source) * rows, rows)
        return outs[w].at[j, pl.ds(start, rows)]

    def own(c, target, s):
        w, j = blocks[c]
        return ins[w].at[s, target * local_experts + j]

    def relay(c, source, s):
        w, j = blocks[c]
        return relays[w].at[j, source, s]

    def tp_copy(c, d, s, to_out):
        target = lax.rem(t + d, tp)
        return pltpu.make_async_remote_copy(
            src_ref=own(c, target, s),
            dst_ref=out_rows(c, g, f) if to_out else relay(c, t, s),
            send_sem=tp_send.at[c, d, s],
            recv_sem=tp_recv.at[c, d, s],
            device_id={"tp": target},
            device_id_type=MESH,
        )

    def fs_copy(c, d, s, src, target):
        return pltpu.make_async_remote_copy(
            src_ref=src,
            dst_ref=out_rows(c, g, f),
            send_sem=fs_send.at[c, d, s],
            recv_sem=fs_recv.at[c, f],
            device_id={"fs": target},
            device_id_type=MESH,
        )

    def gr_copy(c, n, source, src):
        return pltpu.make_async_remote_copy(
            src_ref=src,
            dst_ref=out_rows(c, g, source),
            send_sem=gr_send.at[c, n, source],
            recv_sem=gr_recv.at[c, n, source],
            device_id={"gr": lax.rem(g + n, gr)},
            device_id_type=MESH,
        )

    def to_groups(c, source, src):
        for n in range(1, gr):
            gr_copy(c, n, source, src).start()

    def tp_start(c):
        for d in range(1, tp):
            for s in range(sub):

                @pl.when(t * sub + s == f)
                def _():
                    tp_copy(c, d, s, True).start()

                @pl.when(t * sub + s != f)
                def _():
                    tp_copy(c, d, s, False).start()

    def own_start(c):
        for s in range(sub):
            target = t * sub + s

            @pl.when(target != f)
            def _():
                fs_copy(c, 0, s, own(c, t, s), target).start()

            @pl.when(target == f)
            def _():
                pltpu.make_async_copy(own(c, t, s), bounce.at[c], load_sem.at[c]).start()
                to_groups(c, f, own(c, t, s))

    def own_store(c):
        for s in range(sub):

            @pl.when(t * sub + s == f)
            def _():
                pltpu.make_async_copy(own(c, t, s), bounce.at[c], load_sem.at[c]).wait()
                pltpu.make_async_copy(bounce.at[c], out_rows(c, g, f), store_sem.at[c]).start()

    def tp_arrived(c):
        for d in range(1, tp):
            source = lax.rem(t + tp - d, tp)
            for s in range(sub):
                target = source * sub + s

                @pl.when(target == f)
                def _():
                    tp_copy(c, d, s, True).wait_recv()
                    to_groups(c, f, out_rows(c, g, f))

                @pl.when(target != f)
                def _():
                    pltpu.make_async_remote_copy(
                        src_ref=own(c, t, s),
                        dst_ref=relay(c, source, s),
                        send_sem=tp_send.at[c, d, s],
                        recv_sem=tp_recv.at[c, d, s],
                        device_id={"tp": source},
                        device_id_type=MESH,
                    ).wait_recv()
                    fs_copy(c, d, s, relay(c, source, s), target).start()

    def fs_arrived(c):
        for d in range(1, fs):
            source = lax.rem(f + d, fs)
            pltpu.make_async_remote_copy(
                src_ref=own(c, t, 0),
                dst_ref=out_rows(c, g, source),
                send_sem=fs_send.at[c, 0, 0],
                recv_sem=fs_recv.at[c, source],
                device_id={"fs": source},
                device_id_type=MESH,
            ).wait_recv()
            to_groups(c, source, out_rows(c, g, source))

    total = len(blocks)
    ahead = min(3, total)
    own_start(0)
    for c in range(ahead):
        tp_start(c)
    for c in range(total + 1):
        if c + ahead < total:
            tp_start(c + ahead)
        if c + 1 < total:
            own_start(c + 1)
        if c < total:
            own_store(c)
            tp_arrived(c)
        if c >= 1:
            fs_arrived(c - 1)

    for c in range(total):
        for n in range(1, gr):
            for source in range(fs):
                group = lax.rem(g + gr - n, gr)
                pltpu.make_async_remote_copy(
                    src_ref=own(c, t, 0),
                    dst_ref=out_rows(c, group, source),
                    send_sem=gr_send.at[c, n, source],
                    recv_sem=gr_recv.at[c, n, source],
                    device_id={"gr": group},
                    device_id_type=MESH,
                ).wait_recv()
                gr_copy(c, n, source, out_rows(c, g, source)).wait_send()
        for s in range(sub):
            for d in range(1, tp):
                tp_copy(c, d, s, False).wait_send()
            for d in range(tp):
                target = lax.rem(t + tp - d, tp) * sub + s

                @pl.when(target != f)
                def _():
                    fs_copy(c, d, s, own(c, t, s), target).wait_send()

            @pl.when(t * sub + s == f)
            def _():
                pltpu.make_async_copy(bounce.at[c], out_rows(c, g, f), store_sem.at[c]).wait()


def spread(*weights):
    gr, fs, tp = lax.axis_size("gr"), lax.axis_size("fs"), lax.axis_size("tp")
    experts, rows, columns = weights[0].shape
    local_experts = experts // tp
    assert fs % tp == 0
    sub = fs // tp
    width = columns // sub
    count = len(weights)
    total = count * local_experts
    parts = [w.reshape(experts, rows, sub, width).transpose(2, 0, 1, 3) for w in weights]
    served = jax.ShapeDtypeStruct((local_experts, gr * fs * rows, width), jnp.bfloat16)
    relayed = jax.ShapeDtypeStruct((local_experts, tp, sub, rows, width), jnp.bfloat16)
    dma = pltpu.SemaphoreType.DMA
    sent = 2 * total * rows * columns * (tp - 1 + fs - 1 + (gr - 1) * fs) // fs
    found = pl.pallas_call(
        functools.partial(spread_kernel, (gr, fs, tp, sub, local_experts, rows), count),
        out_shape=[served] * count + [relayed] * count,
        in_specs=[pl.BlockSpec(memory_space=pl.ANY)] * count,
        out_specs=[pl.BlockSpec(memory_space=pl.ANY)] * (2 * count),
        scratch_shapes=[
            pltpu.VMEM((total, rows, width), jnp.bfloat16),
            dma((total, tp, sub)),
            dma((total, tp, sub)),
            dma((total, tp, sub)),
            dma((total, fs)),
            dma((total, gr, fs)),
            dma((total, gr, fs)),
            dma((total,)),
            dma((total,)),
        ],
        compiler_params=pltpu.CompilerParams(collective_id=0, has_side_effects=True),
        cost_estimate=pl.CostEstimate(flops=0, bytes_accessed=40 * sent, transcendentals=0),
    )(*parts)
    return found[:count]


def local(tokens, routes, route_weight, norm_gain, gate_master, up_master, down_master):
    experts = gate_master.shape[0]
    tp_count = lax.axis_size("tp")
    fs_count = lax.axis_size("fs")
    local_experts = experts // tp_count
    token_rows = tokens.shape[0]
    model_width = tokens.shape[1] * fs_count
    capacity = 3 * token_rows // experts
    scaled_gain = norm_gain[None, :, None]
    gate_w = (gate_master * scaled_gain).astype(jnp.bfloat16)
    up_w = (up_master * scaled_gain).astype(jnp.bfloat16)
    down_w = down_master.astype(jnp.bfloat16)
    gate_w, up_w, down_w = spread(gate_w, up_w, down_w)
    as_float = tokens.astype(jnp.float32)
    square_total = lax.psum(jnp.sum(as_float * as_float, axis=1), "fs")
    normed = (as_float * lax.rsqrt(square_total / model_width + norm_eps)[:, None]).astype(
        jnp.bfloat16
    )
    placing = slot_table(routes, experts, capacity)
    slot_rows = jnp.arange(experts * capacity, dtype=jnp.int32)
    picked = (slot_rows[:, None] == placing[None, :]).reshape(experts * capacity, token_rows, 2)
    route_table = jnp.sum(picked.astype(jnp.float32), axis=2).astype(jnp.bfloat16)
    outgoing = jnp.dot(route_table, normed, preferred_element_type=jnp.float32).astype(jnp.bfloat16)
    outgoing = outgoing.reshape(tp_count, local_experts, capacity, tokens.shape[1])
    shard_piece = lax.all_gather(
        lax.all_to_all(outgoing, "tp", split_axis=0, concat_axis=0, tiled=True),
        "fs",
        axis=3,
        tiled=True,
    )
    gate_acc = jnp.einsum("sjcd,jdf->sjcf", shard_piece, gate_w, preferred_element_type=jnp.float32)
    up_acc = jnp.einsum("sjcd,jdf->sjcf", shard_piece, up_w, preferred_element_type=jnp.float32)
    hidden = (jax.nn.silu(gate_acc) * up_acc).astype(jnp.bfloat16)
    partial_value = jnp.einsum("sjcf,jdf->sjcd", hidden, down_w, preferred_element_type=jnp.float32)
    summed = lax.psum_scatter(
        partial_value.astype(jnp.bfloat16), "fs", scatter_dimension=3, tiled=True
    )
    produced = lax.all_to_all(summed, "tp", split_axis=0, concat_axis=0, tiled=True)
    produced = produced.reshape(experts * capacity, produced.shape[3])
    pair_slots = placing.reshape(token_rows, 2)
    first_rows = jnp.take(produced, pair_slots[:, 0], axis=0)
    second_rows = jnp.take(produced, pair_slots[:, 1], axis=0)
    mixed_out = first_rows * route_weight[:, 0:1] + second_rows * route_weight[:, 1:2]
    return (mixed_out.astype(jnp.bfloat16), gate_w, up_w, down_w)


def solution(mesh):
    placed = (
        P(("gr", "tp"), "fs"),
        P(("gr", "tp"), None),
        P(("gr", "tp"), None),
        P(("gr", "fs")),
        P(None, ("gr", "fs"), "tp"),
        P(None, ("gr", "fs"), "tp"),
        P(None, ("gr", "fs"), "tp"),
    )
    return jax.shard_map(
        local,
        mesh=mesh,
        in_specs=placed,
        out_specs=(
            P(("gr", "tp"), "fs"),
            P("tp", None, "fs"),
            P("tp", None, "fs"),
            P("tp", None, "fs"),
        ),
        check_vma=False,
    )
```

```python
import functools

import jax
import jax.numpy as jnp
from jax import lax
from jax.experimental import pallas as pl
from jax.experimental.pallas import tpu as pltpu
from jax.sharding import PartitionSpec as P

norm_eps = 1e-06
MESH = pl.DeviceIdType.MESH


def slot_table(routes, experts, capacity):
    flat_routes = routes.reshape(-1)
    onehot = (flat_routes[:, None] == jnp.arange(experts, dtype=jnp.int32)[None, :]).astype(
        jnp.int32
    )
    running = jnp.cumsum(onehot, axis=0)
    slot_index = jnp.sum(onehot * (running - 1), axis=1)
    return flat_routes * capacity + slot_index


def spread_kernel(sizes, count, flipped, *refs):
    gr, fs, tp, sub, local_experts, rows = sizes
    ins, outs, relays = refs[:count], refs[count : 2 * count], refs[2 * count : 3 * count]
    bounce, tp_send, tp_recv, fs_send, fs_recv, gr_send, gr_recv, load_sem, store_sem = refs[
        3 * count :
    ]
    g, f, t = lax.axis_index("gr"), lax.axis_index("fs"), lax.axis_index("tp")
    blocks = [(w, j) for j in range(local_experts) for w in range(count)]

    barrier = pltpu.get_barrier_semaphore()
    for axis, me, size in (("gr", g, gr), ("fs", f, fs), ("tp", t, tp)):
        for d in range(1, size):
            pl.semaphore_signal(
                barrier, inc=1, device_id={axis: lax.rem(me + d, size)}, device_id_type=MESH
            )
    pl.semaphore_wait(barrier, gr + fs + tp - 3)

    def out_rows(c, group, source):
        w, j = blocks[c]
        start = pl.multiple_of((group * fs + source) * rows, rows)
        if flipped:
            return outs[w].at[j, :, pl.ds(start, rows)]
        return outs[w].at[j, pl.ds(start, rows)]

    def own(c, target, s):
        w, j = blocks[c]
        return ins[w].at[s, target * local_experts + j]

    def relay(c, source, s):
        w, j = blocks[c]
        return relays[w].at[j, source, s]

    def tp_copy(c, d, s, to_out):
        target = lax.rem(t + d, tp)
        return pltpu.make_async_remote_copy(
            src_ref=own(c, target, s),
            dst_ref=out_rows(c, g, f) if to_out else relay(c, t, s),
            send_sem=tp_send.at[c, d, s],
            recv_sem=tp_recv.at[c, d, s],
            device_id={"tp": target},
            device_id_type=MESH,
        )

    def fs_copy(c, d, s, src, target):
        return pltpu.make_async_remote_copy(
            src_ref=src,
            dst_ref=out_rows(c, g, f),
            send_sem=fs_send.at[c, d, s],
            recv_sem=fs_recv.at[c, f],
            device_id={"fs": target},
            device_id_type=MESH,
        )

    def gr_copy(c, n, source, src):
        return pltpu.make_async_remote_copy(
            src_ref=src,
            dst_ref=out_rows(c, g, source),
            send_sem=gr_send.at[c, n, source],
            recv_sem=gr_recv.at[c, n, source],
            device_id={"gr": lax.rem(g + n, gr)},
            device_id_type=MESH,
        )

    def to_groups(c, source, src):
        for n in range(1, gr):
            gr_copy(c, n, source, src).start()

    def tp_start(c):
        for d in range(1, tp):
            for s in range(sub):

                @pl.when(t * sub + s == f)
                def _():
                    tp_copy(c, d, s, True).start()

                @pl.when(t * sub + s != f)
                def _():
                    tp_copy(c, d, s, False).start()

    def own_start(c):
        for s in range(sub):
            target = t * sub + s

            @pl.when(target != f)
            def _():
                fs_copy(c, 0, s, own(c, t, s), target).start()

            @pl.when(target == f)
            def _():
                pltpu.make_async_copy(own(c, t, s), bounce.at[c], load_sem.at[c]).start()
                to_groups(c, f, own(c, t, s))

    def own_store(c):
        for s in range(sub):

            @pl.when(t * sub + s == f)
            def _():
                pltpu.make_async_copy(own(c, t, s), bounce.at[c], load_sem.at[c]).wait()
                pltpu.make_async_copy(bounce.at[c], out_rows(c, g, f), store_sem.at[c]).start()

    def tp_arrived(c):
        for d in range(1, tp):
            source = lax.rem(t + tp - d, tp)
            for s in range(sub):
                target = source * sub + s

                @pl.when(target == f)
                def _():
                    tp_copy(c, d, s, True).wait_recv()
                    to_groups(c, f, out_rows(c, g, f))

                @pl.when(target != f)
                def _():
                    pltpu.make_async_remote_copy(
                        src_ref=own(c, t, s),
                        dst_ref=relay(c, source, s),
                        send_sem=tp_send.at[c, d, s],
                        recv_sem=tp_recv.at[c, d, s],
                        device_id={"tp": source},
                        device_id_type=MESH,
                    ).wait_recv()
                    fs_copy(c, d, s, relay(c, source, s), target).start()

    def fs_arrived(c):
        for d in range(1, fs):
            source = lax.rem(f + d, fs)
            pltpu.make_async_remote_copy(
                src_ref=own(c, t, 0),
                dst_ref=out_rows(c, g, source),
                send_sem=fs_send.at[c, 0, 0],
                recv_sem=fs_recv.at[c, source],
                device_id={"fs": source},
                device_id_type=MESH,
            ).wait_recv()
            to_groups(c, source, out_rows(c, g, source))

    total = len(blocks)
    ahead = min(3, total)
    own_start(0)
    for c in range(ahead):
        tp_start(c)
    for c in range(total + 1):
        if c + ahead < total:
            tp_start(c + ahead)
        if c + 1 < total:
            own_start(c + 1)
        if c < total:
            own_store(c)
            tp_arrived(c)
        if c >= 1:
            fs_arrived(c - 1)

    for c in range(total):
        for n in range(1, gr):
            for source in range(fs):
                group = lax.rem(g + gr - n, gr)
                pltpu.make_async_remote_copy(
                    src_ref=own(c, t, 0),
                    dst_ref=out_rows(c, group, source),
                    send_sem=gr_send.at[c, n, source],
                    recv_sem=gr_recv.at[c, n, source],
                    device_id={"gr": group},
                    device_id_type=MESH,
                ).wait_recv()
                gr_copy(c, n, source, out_rows(c, g, source)).wait_send()
        for s in range(sub):
            for d in range(1, tp):
                tp_copy(c, d, s, False).wait_send()
            for d in range(tp):
                target = lax.rem(t + tp - d, tp) * sub + s

                @pl.when(target != f)
                def _():
                    fs_copy(c, d, s, own(c, t, s), target).wait_send()

            @pl.when(t * sub + s == f)
            def _():
                pltpu.make_async_copy(bounce.at[c], out_rows(c, g, f), store_sem.at[c]).wait()


def spread(*weights):
    gr, fs, tp = lax.axis_size("gr"), lax.axis_size("fs"), lax.axis_size("tp")
    experts, rows, columns = weights[0].shape
    local_experts = experts // tp
    assert fs % tp == 0
    sub = fs // tp
    width = columns // sub
    count = len(weights)
    total = count * local_experts
    flipped = rows % 128 == 0
    order = (2, 0, 3, 1) if flipped else (2, 0, 1, 3)
    parts = [w.reshape(experts, rows, sub, width).transpose(order) for w in weights]
    block = (width, rows) if flipped else (rows, width)
    whole = (width, gr * fs * rows) if flipped else (gr * fs * rows, width)
    served = jax.ShapeDtypeStruct((local_experts, *whole), jnp.bfloat16)
    relayed = jax.ShapeDtypeStruct((local_experts, tp, sub, *block), jnp.bfloat16)
    dma = pltpu.SemaphoreType.DMA
    sent = 2 * total * rows * columns * (tp - 1 + fs - 1 + (gr - 1) * fs) // fs
    found = pl.pallas_call(
        functools.partial(spread_kernel, (gr, fs, tp, sub, local_experts, rows), count, flipped),
        out_shape=[served] * count + [relayed] * count,
        in_specs=[pl.BlockSpec(memory_space=pl.ANY)] * count,
        out_specs=[pl.BlockSpec(memory_space=pl.ANY)] * (2 * count),
        scratch_shapes=[
            pltpu.VMEM((total, *block), jnp.bfloat16),
            dma((total, tp, sub)),
            dma((total, tp, sub)),
            dma((total, tp, sub)),
            dma((total, fs)),
            dma((total, gr, fs)),
            dma((total, gr, fs)),
            dma((total,)),
            dma((total,)),
        ],
        compiler_params=pltpu.CompilerParams(collective_id=0, has_side_effects=True),
        cost_estimate=pl.CostEstimate(flops=0, bytes_accessed=40 * sent, transcendentals=0),
    )(*parts)
    return [w.swapaxes(1, 2) if flipped else w for w in found[:count]]


def local(tokens, routes, route_weight, norm_gain, gate_master, up_master, down_master):
    experts = gate_master.shape[0]
    tp_count = lax.axis_size("tp")
    fs_count = lax.axis_size("fs")
    local_experts = experts // tp_count
    token_rows = tokens.shape[0]
    model_width = tokens.shape[1] * fs_count
    capacity = 3 * token_rows // experts
    scaled_gain = norm_gain[None, :, None]
    gate_w = (gate_master * scaled_gain).astype(jnp.bfloat16)
    up_w = (up_master * scaled_gain).astype(jnp.bfloat16)
    down_w = down_master.astype(jnp.bfloat16)
    gate_w, up_w, down_w = spread(gate_w, up_w, down_w)
    as_float = tokens.astype(jnp.float32)
    square_total = lax.psum(jnp.sum(as_float * as_float, axis=1), "fs")
    normed = (as_float * lax.rsqrt(square_total / model_width + norm_eps)[:, None]).astype(
        jnp.bfloat16
    )
    placing = slot_table(routes, experts, capacity)
    slot_rows = jnp.arange(experts * capacity, dtype=jnp.int32)
    picked = (slot_rows[:, None] == placing[None, :]).reshape(experts * capacity, token_rows, 2)
    route_table = jnp.sum(picked.astype(jnp.float32), axis=2).astype(jnp.bfloat16)
    outgoing = jnp.dot(route_table, normed, preferred_element_type=jnp.float32).astype(jnp.bfloat16)
    outgoing = outgoing.reshape(tp_count, local_experts, capacity, tokens.shape[1])
    shard_piece = lax.all_gather(
        lax.all_to_all(outgoing, "tp", split_axis=0, concat_axis=0, tiled=True),
        "fs",
        axis=3,
        tiled=True,
    )
    returned = []
    for j in range(local_experts):
        rows = shard_piece[:, j]
        gate_acc = jnp.einsum("scd,df->scf", rows, gate_w[j], preferred_element_type=jnp.float32)
        up_acc = jnp.einsum("scd,df->scf", rows, up_w[j], preferred_element_type=jnp.float32)
        hidden = (jax.nn.silu(gate_acc) * up_acc).astype(jnp.bfloat16)
        partial_value = jnp.einsum(
            "scf,df->scd", hidden, down_w[j], preferred_element_type=jnp.float32
        )
        summed = lax.psum_scatter(
            partial_value.astype(jnp.bfloat16), "fs", scatter_dimension=2, tiled=True
        )
        returned.append(lax.all_to_all(summed, "tp", split_axis=0, concat_axis=0, tiled=True))
    produced = jnp.stack(returned, axis=1)
    produced = produced.reshape(experts * capacity, produced.shape[3])
    pair_slots = placing.reshape(token_rows, 2)
    first_rows = jnp.take(produced, pair_slots[:, 0], axis=0)
    second_rows = jnp.take(produced, pair_slots[:, 1], axis=0)
    mixed_out = first_rows * route_weight[:, 0:1] + second_rows * route_weight[:, 1:2]
    return (mixed_out.astype(jnp.bfloat16), gate_w, up_w, down_w)


def solution(mesh):
    placed = (
        P(("gr", "tp"), "fs"),
        P(("gr", "tp"), None),
        P(("gr", "tp"), None),
        P(("gr", "fs")),
        P(None, ("gr", "fs"), "tp"),
        P(None, ("gr", "fs"), "tp"),
        P(None, ("gr", "fs"), "tp"),
    )
    return jax.shard_map(
        local,
        mesh=mesh,
        in_specs=placed,
        out_specs=(
            P(("gr", "tp"), "fs"),
            P("tp", None, "fs"),
            P("tp", None, "fs"),
            P("tp", None, "fs"),
        ),
        check_vma=False,
    )
```
